32 devices in a mesh: ep: 8 (over z, x), tp: 4 (over y, core).
Axes of the slice: x: 2, y: 2, z: 4, core: 2. Of those that a mesh axis runs over, the one named last changes fastest.
Arguments:
- mix_in: bfloat16 [4096, 2048], P('ep'), may hold values from -6 to 6
- forget_shift: float32 [4096], P('ep'), may hold values from -2.5 to 2.5, as said below
- mix_gain: float32 [2048], replicated, may hold values from 0.1 to 1.9
- w_query: bfloat16 [2048, 1024], P(None, 'tp'), may hold values from -0.125 to 0.125
- w_forget: bfloat16 [2048, 1024], P(None, 'tp'), may hold values from -0.125 to 0.125
- w_value: bfloat16 [2048, 1024], P(None, 'tp'), may hold values from -0.125 to 0.125
- forget_room: float32 [1024], P('tp'), may hold values from 0 to 1, as said below
- head_gain: float32 [1024], P('tp'), may hold values from 0.1 to 1.9
- w_out: bfloat16 [1024, 2048], P('tp'), may hold values from -0.1875 to 0.1875
- moe_in: bfloat16 [2048, 2048], P('ep'), may hold values from -6 to 6
- moe_gain: float32 [2048], replicated, may hold values from 0.1 to 1.9
- expert_choice: int32 [2048, 4], P('ep'), may hold values from 0 to 7, as said below
- route_logit: float32 [2048, 4], P(('ep', 'tp')), may hold values from -6 to 6
- w_exp_gate: bfloat16 [8, 2048, 1024], P('ep', None, 'tp'), may hold values from -0.125 to 0.125
- w_exp_up: bfloat16 [8, 2048, 1024], P('ep', None, 'tp'), may hold values from -0.125 to 0.125
- w_exp_down: bfloat16 [8, 1024, 2048], P('ep', 'tp'), may hold values from -0.1875 to 0.1875
- w_sh_gate: bfloat16 [2048, 512], P(None, 'tp'), may hold values from -0.125 to 0.125
- w_sh_up: bfloat16 [2048, 512], P(None, 'tp'), may hold values from -0.125 to 0.125
- w_sh_down: bfloat16 [512, 2048], P('tp'), may hold values from -0.25 to 0.25
Outputs:
- mixer_out: bfloat16 [4096, 2048], P(('ep', 'tp'))
- moe_out: bfloat16 [2048, 2048], P(('ep', 'tp'))
The draws below stay inside these ranges and needn't reach their ends.
Inputs may be any that keep to these rules, and one draw needn't show every extreme that they name: `forget_room`: positive and at most 1/6 in every entry. `forget_shift`: constant over each aligned span of 64 positions. `expert_choice`: each row names 4 different experts. In each aligned block of 64 rows no expert is named by more than 48 rows; in every draw one expert is named by exactly 48 rows in every block.
All inputs are finite; a program needn't handle non-finite values.
Results may differ from the reference program's by a relative error of at most 0.02.
Values may be sent and summed in bfloat16 or wider, within the bound.
A program may use at most 128 MiB of HBM per device.

```python
import jax
import jax.numpy as jnp
from jax import lax

D = 2048
HEADS = 16
HEAD_K = 64
HEAD_V = 64
MIX_K = 1024
MIX_W = 1024
SPAN = 64
MIX_DEV = 512
LENGTH = 4096
TOK_MOE = 2048
QUARTER = 64
EXPERTS = 8
TOP_K = 4
EXP_FF = 1024
SHARED_FF = 512
MEAN_LOAD = 32
CAP = 48
N_EP = 8
N_TP = 4


def draw_forget_room(key, part):
    keys = jax.random.split(key, 2)
    slow_share = 0.5
    is_slow = jax.random.uniform(keys[0], (HEADS,), jnp.float32) < slow_share
    spread = jax.random.uniform(keys[1], (HEADS, HEAD_K), jnp.float32)
    slow_room = jnp.exp(jnp.log(0.3) + spread * (jnp.log(2.0) - jnp.log(0.3))) / LENGTH
    fast_room = jnp.exp(jnp.log(1.0 / 16.0) + spread * (jnp.log(1.0 / 6.0) - jnp.log(1.0 / 16.0)))
    return jnp.where(is_slow[:, None], slow_room, fast_room).reshape(-1).astype(jnp.float32)


def draw_forget_shift(key, part):
    keys = jax.random.split(key, 2)
    device_part = jax.random.uniform(keys[0], (LENGTH // MIX_DEV,), jnp.float32, -1.5, 1.5)
    block_part = jax.random.uniform(keys[1], (LENGTH // SPAN,), jnp.float32, -1.0, 1.0)
    shifted = jnp.repeat(device_part, MIX_DEV) + jnp.repeat(block_part, SPAN)
    return shifted.astype(jnp.float32)


def draw_expert_choice(key, part):
    blocks = TOK_MOE // QUARTER
    half_load = MEAN_LOAD // 2
    keys = jax.random.split(key, 2)
    fullest = jax.random.randint(keys[0], (), 0, EXPERTS)

    def one_block(block_key):
        inner_keys = jax.random.split(block_key, 3)
        expert_ids = jnp.arange(EXPERTS, dtype=jnp.int32)
        ranking = jax.random.randint(inner_keys[0], (EXPERTS,), 0, 1 << 20) * EXPERTS + expert_ids
        ranking = jnp.where(expert_ids == fullest, -1, ranking)
        ordering = jnp.argsort(ranking)
        offsets = jax.random.randint(inner_keys[1], (EXPERTS // 2,), -half_load, half_load + 1)
        offsets = offsets.at[0].set(half_load)
        counts = MEAN_LOAD + jnp.stack([offsets, -offsets], axis=1).reshape(-1)
        labels = jnp.repeat(ordering, counts, total_repeat_length=QUARTER * TOP_K)
        table = labels.reshape(TOP_K, QUARTER).T
        shuffle = jax.random.permutation(inner_keys[2], QUARTER)
        return table[shuffle]
    block_keys = jax.random.split(keys[1], blocks)
    chosen = jax.vmap(one_block)(block_keys)
    return chosen.reshape(blocks * QUARTER, TOP_K).astype(jnp.int32)


def shard_levels(key, dims, cuts, smallest, top_value):
    factor_of = 1.0
    for axis_at, parts in cuts:
        draws = jax.random.uniform(jax.random.fold_in(jax.random.fold_in(key, 6), axis_at), (parts,), jnp.float32, smallest / len(cuts), top_value / len(cuts))
        factor_of = factor_of * jnp.repeat(jnp.exp(draws), dims[axis_at] // parts).reshape((-1,) + (1,) * (len(dims) - 1 - axis_at))
    return factor_of


def centred(rng, shape, scale, most, cuts=(), held_as=jnp.bfloat16):
    loudness = shard_levels(rng, shape, cuts, -0.22, 0.18) if cuts else 1.0
    array = jax.random.normal(rng, shape, jnp.float32) * scale * loudness
    return jnp.minimum(jnp.maximum(array, -most), most).astype(held_as)


def setup_inputs(seed: int = 0) -> dict:
    key_list = jax.random.split(jax.random.key(seed), 20)
    return {
        "mix_in": centred(key_list[0], (LENGTH, D), 1.0, 6.0, ((0, 8),)),
        "forget_shift": draw_forget_shift(jax.random.fold_in(key_list[19], 71), 0),
        "mix_gain": jnp.clip(1.0 + 0.18 * jax.random.normal(key_list[2], (D,), jnp.float32), 0.1, 1.9),
        "w_query": centred(key_list[3], (D, MIX_K), D ** -0.5, 0.125, ((1, 4),)),
        "w_forget": centred(key_list[4], (D, MIX_K), D ** -0.5, 0.125, ((1, 4),)),
        "w_value": centred(key_list[5], (D, MIX_W), D ** -0.5, 0.125, ((1, 4),)),
        "forget_room": draw_forget_room(jax.random.fold_in(key_list[19], 71), 0),
        "head_gain": jnp.clip(1.0 + 0.18 * jax.random.normal(key_list[7], (MIX_W,), jnp.float32), 0.1, 1.9),
        "w_out": centred(key_list[8], (MIX_W, D), MIX_W ** -0.5, 0.1875, ((0, 4),)),
        "moe_in": centred(key_list[9], (TOK_MOE, D), 1.0, 6.0, ((0, 8),)),
        "moe_gain": jnp.clip(1.0 + 0.18 * jax.random.normal(key_list[10], (D,), jnp.float32), 0.1, 1.9),
        "expert_choice": draw_expert_choice(jax.random.fold_in(key_list[19], 71), 0),
        "route_logit": centred(key_list[12], (TOK_MOE, TOP_K), 1.5, 6.0, ((0, 32),), jnp.float32),
        "w_exp_gate": centred(key_list[13], (EXPERTS, D, EXP_FF), D ** -0.5, 0.125, ((0, 8), (2, 4))),
        "w_exp_up": centred(key_list[14], (EXPERTS, D, EXP_FF), D ** -0.5, 0.125, ((0, 8), (2, 4))),
        "w_exp_down": centred(key_list[15], (EXPERTS, EXP_FF, D), EXP_FF ** -0.5, 0.1875, ((0, 8), (1, 4))),
        "w_sh_gate": centred(key_list[16], (D, SHARED_FF), D ** -0.5, 0.125, ((1, 4),)),
        "w_sh_up": centred(key_list[17], (D, SHARED_FF), D ** -0.5, 0.125, ((1, 4),)),
        "w_sh_down": centred(key_list[18], (SHARED_FF, D), SHARED_FF ** -0.5, 0.25, ((0, 4),)),
    }


epsilon = 1e-06
route_scale = 2.5
highest = lax.Precision.HIGHEST

def norm_rows(row_data, gain_vec):
    widened = row_data.astype(jnp.float32)
    scaled = widened * lax.rsqrt(lax.optimization_barrier(jnp.mean(widened * widened, axis=-1, keepdims=True)) + epsilon)
    return (scaled * gain_vec).astype(jnp.bfloat16)

def block_terms(queries, keyed, log_forget, values, span_len):
    token_count, head_count, key_width = queries.shape
    blocks = token_count // span_len
    key_shape = (blocks, span_len, head_count, key_width)
    queries = queries.reshape(key_shape)
    keyed = keyed.reshape(key_shape)
    log_forget = log_forget.reshape(key_shape)
    values = values.reshape(blocks, span_len, head_count, values.shape[-1])
    log_decay = jnp.cumsum(log_forget, axis=1)
    middle = log_decay[:, span_len // 2:span_len // 2 + 1]
    block_end = log_decay[:, span_len - 1:]
    scores = jnp.einsum('nthd,nshd->nhts', queries * jnp.exp(log_decay - middle), keyed * jnp.exp(middle - log_decay), precision=highest)
    causal = jnp.arange(span_len)[:, None] >= jnp.arange(span_len)[None, :]
    scores = jnp.where(causal, scores, 0.0)
    within = jnp.einsum('nhts,nshv->nthv', scores, values, precision=highest)
    query_decay = queries * jnp.exp(log_decay)
    decay_total = jnp.exp(block_end[:, 0])
    state_added = jnp.einsum('nshd,nshv->nhdv', keyed * jnp.exp(block_end - log_decay), values, precision=highest)
    return (within, query_decay, decay_total, state_added)

def split_sum(left, right, groups):
    group_width = left.shape[1] // groups
    running = jnp.zeros((left.shape[0], right.shape[1]), jnp.float32)
    for member in range(groups):
        partial_value = jnp.dot(left[:, member * group_width:(member + 1) * group_width], right[member * group_width:(member + 1) * group_width], preferred_element_type=jnp.float32)
        rounded = lax.optimization_barrier(partial_value.astype(jnp.bfloat16))
        running = running + rounded.astype(jnp.float32)
    return running

def mixer_heads(mix_in, forget_shift, mix_gain, w_query, w_forget, w_value, forget_room, head_gain):
    normed = norm_rows(mix_in, mix_gain)
    queries = jax.nn.silu(jnp.dot(normed, w_query, preferred_element_type=jnp.float32))
    before = jnp.dot(normed, w_forget, preferred_element_type=jnp.float32) + forget_shift[:, None]
    values = jnp.dot(normed, w_value, preferred_element_type=jnp.float32)
    forget_rate = forget_room * jax.nn.sigmoid(-before)
    log_forget = jnp.log1p(-forget_rate)
    token_count = normed.shape[0]
    head_count = values.shape[1] // HEAD_V
    key_shape = (token_count, head_count, HEAD_K)
    within, query_decay, decay_total, state_added = block_terms(queries.reshape(key_shape), forget_rate.reshape(key_shape), log_forget.reshape(key_shape), values.reshape(token_count, head_count, HEAD_V), SPAN)

    def advance(state_now, pieces):
        return (pieces[0][..., None] * state_now + pieces[1], state_now)
    zero_state = jnp.zeros(state_added.shape[1:], jnp.float32)
    state_in = lax.scan(advance, zero_state, (decay_total, state_added))[1]
    mixed = within + jnp.einsum('nthd,nhdv->nthv', query_decay, state_in, precision=highest)
    mixed = mixed.reshape(token_count, head_count, HEAD_V)
    normal = mixed * lax.rsqrt(lax.optimization_barrier(jnp.mean(mixed * mixed, axis=-1, keepdims=True)) + epsilon)
    head_out = (normal * head_gain.reshape(head_count, HEAD_V)).astype(jnp.bfloat16)
    return head_out.reshape(token_count, head_count * HEAD_V)

def experts_out(hidden, expert_choice, weights, w_exp_gate, w_exp_up, w_exp_down):
    token_count = hidden.shape[0]
    slot_limit = N_TP * N_EP * CAP
    flat_ids = expert_choice.reshape(-1)
    flat_tokens = (jnp.arange(flat_ids.shape[0]) // TOP_K).astype(jnp.int32)
    flat_weights = weights.reshape(-1)
    padded = jnp.concatenate([hidden, jnp.zeros((1, hidden.shape[1]), jnp.bfloat16)], axis=0)

    def one_expert(running, pieces):
        expert_index, gate_weight, up_weight, down_weight = pieces
        chosen = flat_ids == expert_index
        places = jnp.where(chosen, jnp.cumsum(chosen.astype(jnp.int32)) - 1, slot_limit).astype(jnp.int32)
        source = jnp.full((slot_limit,), token_count, jnp.int32).at[places].set(flat_tokens, mode='drop')
        slot_weight = jnp.zeros((slot_limit,), jnp.float32).at[places].set(flat_weights, mode='drop')
        gathered = padded[source]
        gate_pre = jnp.dot(gathered, gate_weight, preferred_element_type=jnp.float32)
        up_pre = jnp.dot(gathered, up_weight, preferred_element_type=jnp.float32)
        activations = (jax.nn.silu(gate_pre) * up_pre).astype(jnp.bfloat16)
        outcome = split_sum(activations, down_weight, N_TP).astype(jnp.bfloat16)
        running = running.at[source].add(slot_weight[:, None] * outcome.astype(jnp.float32), mode='drop')
        return (running, None)
    start_sum = jnp.zeros(hidden.shape, jnp.float32)
    expert_ids = jnp.arange(w_exp_gate.shape[0], dtype=jnp.int32)
    return lax.scan(one_expert, start_sum, (expert_ids, w_exp_gate, w_exp_up, w_exp_down))[0]

def reference(mix_in, forget_shift, mix_gain, w_query, w_forget, w_value, forget_room, head_gain, w_out, moe_in, moe_gain, expert_choice, route_logit, w_exp_gate, w_exp_up, w_exp_down, w_sh_gate, w_sh_up, w_sh_down):
    head_out = mixer_heads(mix_in, forget_shift, mix_gain, w_query, w_forget, w_value, forget_room, head_gain)
    mixer_out = split_sum(head_out, w_out, N_TP).astype(jnp.bfloat16)
    hidden = norm_rows(moe_in, moe_gain)
    chance = jax.nn.sigmoid(route_logit)
    weights = chance / lax.optimization_barrier(jnp.sum(chance, axis=-1, keepdims=True)) * route_scale
    routed = experts_out(hidden, expert_choice, weights, w_exp_gate, w_exp_up, w_exp_down)
    shared_gate = jnp.dot(hidden, w_sh_gate, preferred_element_type=jnp.float32)
    shared_up = jnp.dot(hidden, w_sh_up, preferred_element_type=jnp.float32)
    shared_act = (jax.nn.silu(shared_gate) * shared_up).astype(jnp.bfloat16)
    shared_sum = split_sum(shared_act, w_sh_down, N_TP)
    moe_out = (routed + shared_sum).astype(jnp.bfloat16)
    return (mixer_out, moe_out)
```

```python
import functools

import jax
import jax.numpy as jnp
from jax import lax
from jax.experimental import pallas as pl
from jax.experimental.pallas import tpu as pltpu
from jax.sharding import PartitionSpec as P

HEAD = 64
SPAN = 64
ROW_BLOCK = 512

epsilon = 1e-06
route_scale = 2.5


NT = (((1,), (1,)), ((), ()))
TN = (((0,), (0,)), ((), ()))
NN = (((1,), (0,)), ((), ()))


def dot(a, b, dims=NN):
    return lax.dot_general(
        a.astype(jnp.bfloat16),
        b.astype(jnp.bfloat16),
        dims,
        preferred_element_type=jnp.float32,
    )


def two_part(x):
    high = x.astype(jnp.bfloat16)
    return high, (x - high.astype(jnp.float32)).astype(jnp.bfloat16)


def head_mask(rows, columns):
    row = lax.broadcasted_iota(jnp.int32, (rows, columns), 0) // HEAD
    column = lax.broadcasted_iota(jnp.int32, (rows, columns), 1) // HEAD
    return row == column


def norm_rows(row_data, gain_vec):
    widened = row_data.astype(jnp.float32)
    scaled = widened * lax.rsqrt(jnp.mean(widened * widened, axis=-1, keepdims=True) + epsilon)
    return (scaled * gain_vec).astype(jnp.bfloat16)


def local_scan(
    x_ref, shift_ref, gain_ref, wq_ref, wf_ref, wv_ref, room_ref,
    mixed_ref, query_ref, carry_ref, state, decay,
):
    step = pl.program_id(0)
    width = wq_ref.shape[1]
    heads = width // HEAD

    @pl.when(step == 0)
    def _():
        state[...] = jnp.zeros_like(state)
        decay[...] = jnp.ones_like(decay)

    normed = norm_rows(x_ref[...], gain_ref[...])
    queries = dot(normed, wq_ref[...])
    queries = queries / (1.0 + jnp.exp(-queries))
    before = dot(normed, wf_ref[...]) + shift_ref[...]
    values = dot(normed, wv_ref[...])
    rate = room_ref[...] / (1.0 + jnp.exp(before))
    log_forget = jnp.log1p(-rate)
    causal = (
        lax.broadcasted_iota(jnp.int32, (SPAN, SPAN), 0)
        >= lax.broadcasted_iota(jnp.int32, (SPAN, SPAN), 1)
    )
    lower = causal.astype(jnp.bfloat16)
    high, low = two_part(log_forget)
    log_decay = dot(lower, high) + dot(lower, low)
    middle = log_decay[SPAN // 2 : SPAN // 2 + 1]
    block_end = log_decay[SPAN - 1 :]
    left = (queries * jnp.exp(log_decay - middle)).astype(jnp.bfloat16)
    right = rate * jnp.exp(middle - log_decay)
    mask = head_mask(width, width)
    stacked = jnp.concatenate([left] * heads, axis=0)
    stacked = jnp.where(mask, stacked, jnp.zeros_like(stacked))
    scores = dot(stacked, right, NT)
    scores = jnp.where(jnp.concatenate([causal] * heads, axis=0), scores, 0.0)
    spread = jnp.where(mask, dot(scores, values), 0.0)
    within = spread[:SPAN]
    for head in range(1, heads):
        within = within + spread[head * SPAN : (head + 1) * SPAN]
    query_decay = queries * jnp.exp(log_decay)
    mixed_ref[...] = within + dot(query_decay, state[...], NT)
    query_ref[...] = (query_decay * decay[...]).astype(jnp.bfloat16)
    added = dot(values, rate * jnp.exp(block_end - log_decay), TN)
    total = jnp.exp(block_end)
    new_state = total * state[...] + jnp.where(mask, added, 0.0)
    state[...] = new_state
    decay[...] = decay[...] * total

    @pl.when(step == pl.num_programs(0) - 1)
    def _():
        packed = new_state[:HEAD]
        for head in range(1, heads):
            packed = packed + new_state[head * HEAD : (head + 1) * HEAD]
        high, low = two_part(decay[...])
        row = lax.broadcasted_iota(jnp.int32, (16, width), 0)
        tail = jnp.where(row == 0, high.astype(jnp.float32), 0.0)
        tail = jnp.where(row == 1, low.astype(jnp.float32), tail)
        carry_ref[:HEAD] = packed.astype(jnp.bfloat16)
        carry_ref[HEAD:] = tail.astype(jnp.bfloat16)


def finish(
    place_ref, mixed_ref, query_ref, all_ref, gain_ref, out_w_ref, part_ref, start
):
    width = mixed_ref.shape[1]
    heads = width // HEAD
    mask = head_mask(width, width)

    @pl.when(pl.program_id(0) == 0)
    def _():
        def one(lap, state):
            block = all_ref[lap].astype(jnp.float32)
            total = block[HEAD : HEAD + 1] + block[HEAD + 1 : HEAD + 2]
            return total * state + block[:HEAD]

        packed = lax.fori_loop(0, place_ref[0], one, jnp.zeros((HEAD, width), jnp.float32))
        whole = jnp.concatenate([packed] * heads, axis=0)
        start[...] = jnp.where(mask, whole, 0.0).astype(jnp.bfloat16)

    mixed = mixed_ref[...] + dot(query_ref[...], start[...], NT)
    ones = mask.astype(jnp.bfloat16)
    high, low = two_part(mixed * mixed)
    square = (dot(high, ones) + dot(low, ones)) * (1.0 / HEAD)
    head_out = (mixed * lax.rsqrt(square + epsilon) * gain_ref[...]).astype(jnp.bfloat16)
    part_ref[...] = dot(head_out, out_w_ref[...]).astype(jnp.bfloat16)


def whole_block(array):
    return pl.BlockSpec(array.shape, lambda i, rank=array.ndim: (0,) * rank)


def mixer_scan(mix_in, forget_shift, mix_gain, w_query, w_forget, w_value, forget_room):
    rows, width = mix_in.shape[0], w_query.shape[1]
    gain = mix_gain[None]
    room = forget_room[None]
    by_span = lambda columns: pl.BlockSpec((SPAN, columns), lambda i: (i, 0))
    return pl.pallas_call(
        local_scan,
        grid=(rows // SPAN,),
        in_specs=[
            by_span(mix_in.shape[1]), by_span(1), whole_block(gain), whole_block(w_query),
            whole_block(w_forget), whole_block(w_value), whole_block(room),
        ],
        out_specs=[
            by_span(width), by_span(width),
            pl.BlockSpec((HEAD + 16, width), lambda i: (0, 0)),
        ],
        out_shape=[
            jax.ShapeDtypeStruct((rows, width), jnp.float32),
            jax.ShapeDtypeStruct((rows, width), jnp.bfloat16),
            jax.ShapeDtypeStruct((HEAD + 16, width), jnp.bfloat16),
        ],
        scratch_shapes=[
            pltpu.VMEM((width, width), jnp.float32),
            pltpu.VMEM((1, width), jnp.float32),
        ],
        compiler_params=pltpu.CompilerParams(vmem_limit_bytes=32 * 1024 * 1024),
        cost_estimate=pl.CostEstimate(
            flops=40_000_000_000 * rows // 512, bytes_accessed=7_000_000, transcendentals=0
        ),
        name="mixer_scan",
    )(mix_in, forget_shift[:, None], gain, w_query, w_forget, w_value, room)


def mixer_finish(place, mixed, query, carried, head_gain, w_out):
    rows, width = mixed.shape
    block = min(rows, 4 * SPAN)
    gain = head_gain[None]
    by_rows = lambda columns: pl.BlockSpec((block, columns), lambda i: (i, 0))
    return pl.pallas_call(
        finish,
        grid=(rows // block,),
        in_specs=[
            pl.BlockSpec(memory_space=pltpu.SMEM), by_rows(width), by_rows(width),
            whole_block(carried), whole_block(gain), whole_block(w_out),
        ],
        out_specs=by_rows(w_out.shape[1]),
        out_shape=jax.ShapeDtypeStruct((rows, w_out.shape[1]), jnp.bfloat16),
        scratch_shapes=[pltpu.VMEM((width, width), jnp.bfloat16)],
        compiler_params=pltpu.CompilerParams(vmem_limit_bytes=32 * 1024 * 1024),
        cost_estimate=pl.CostEstimate(
            flops=4_000_000_000, bytes_accessed=5_000_000, transcendentals=0
        ),
        name="mixer_finish",
    )(place, mixed, query, carried, gain, w_out)


def swap(x, bit):
    count = lax.axis_size("tp")
    return lax.ppermute(x, "tp", [(i, i ^ bit) for i in range(count)])


def scatter_sum(part, rank):
    count = lax.axis_size("tp")
    rows = part.shape[0] // count
    bit = 1
    while bit < count:
        part = part.reshape(part.shape[0] // (2 * rows), 2, rows, part.shape[-1])
        mine = (rank // bit) % 2
        keep = lax.dynamic_index_in_dim(part, mine, 1, False)
        send = lax.dynamic_index_in_dim(part, 1 - mine, 1, False)
        total = keep.astype(jnp.float32) + swap(send, bit).astype(jnp.float32)
        part = total.reshape(-1, part.shape[-1])
        bit *= 2
        if bit < count:
            part = part.astype(jnp.bfloat16)
    return part


def gather_groups(w):
    count = lax.axis_size("tp")
    held = [w]
    bit = count // 2
    while bit:
        held = held + [swap(x, bit) for x in held]
        bit //= 2
    return held


def local(
    mix_in, forget_shift, mix_gain, w_query, w_forget, w_value, forget_room, head_gain, w_out,
    moe_in, moe_gain, expert_choice, route_logit, w_exp_gate, w_exp_up, w_exp_down,
    w_sh_gate, w_sh_up, w_sh_down,
):
    tp_count = lax.axis_size("tp")
    rank = lax.axis_index("tp")
    place = lax.axis_index("ep")
    local_experts = w_exp_gate.shape[0]
    experts = lax.axis_size("ep") * local_experts
    quarter = moe_in.shape[0] // tp_count
    model = moe_in.shape[1]

    gates = gather_groups(w_exp_gate)
    ups = gather_groups(w_exp_up)
    downs = gather_groups(w_exp_down)

    hidden = norm_rows(moe_in, moe_gain)
    chance = jax.nn.sigmoid(route_logit)
    weights = chance / jnp.sum(chance, axis=-1, keepdims=True) * route_scale
    own_choice = lax.dynamic_slice_in_dim(expert_choice, rank * quarter, quarter, 0)
    table = jnp.sum(
        jnp.where(
            own_choice[..., None] == jnp.arange(experts, dtype=jnp.int32),
            weights[..., None],
            0.0,
        ),
        axis=1,
    )
    high, low = two_part(table)
    spare = -(2 * experts) % 128
    own_rows = lax.dynamic_slice_in_dim(hidden, rank * quarter, quarter, 0)
    sent = jnp.concatenate(
        [own_rows, high, low, jnp.zeros((quarter, spare), jnp.bfloat16)], axis=1
    )
    gathered = lax.all_gather(sent, "ep", axis=0, tiled=True)

    mixed, query, carry = mixer_scan(
        mix_in, forget_shift, mix_gain, w_query, w_forget, w_value, forget_room
    )
    carried = lax.all_gather(carry, "ep")

    rows = gathered[:, :model]
    shares = (
        gathered[:, model : model + experts].astype(jnp.float32)
        + gathered[:, model + experts : model + 2 * experts].astype(jnp.float32)
    )

    def expert_terms(block):
        rows, shares = block
        routed = jnp.zeros(rows.shape, jnp.float32)
        for each in range(local_experts):
            result = jnp.zeros(rows.shape, jnp.float32)
            for gate, up, down in zip(gates, ups, downs):
                act = (
                    jax.nn.silu(jnp.dot(rows, gate[each], preferred_element_type=jnp.float32))
                    * jnp.dot(rows, up[each], preferred_element_type=jnp.float32)
                ).astype(jnp.bfloat16)
                result = result + jnp.dot(act, down[each], preferred_element_type=jnp.float32)
            share = lax.dynamic_slice_in_dim(shares, place * local_experts + each, 1, 1)
            routed = routed + share * result
        return routed.astype(jnp.bfloat16)

    blocks = max(1, rows.shape[0] // ROW_BLOCK)
    if blocks == 1:
        routed = expert_terms((rows, shares))
    else:
        split = lambda x: x.reshape(blocks, x.shape[0] // blocks, x.shape[1])
        routed = lax.map(expert_terms, (split(rows), split(shares))).reshape(rows.shape)
    routed = lax.psum_scatter(
        routed, "ep", scatter_dimension=0, tiled=True
    ).astype(jnp.float32)

    shared_gate = jnp.dot(hidden, w_sh_gate, preferred_element_type=jnp.float32)
    shared_up = jnp.dot(hidden, w_sh_up, preferred_element_type=jnp.float32)
    shared_act = (jax.nn.silu(shared_gate) * shared_up).astype(jnp.bfloat16)
    shared_part = jnp.dot(shared_act, w_sh_down, preferred_element_type=jnp.float32)
    shared_sum = scatter_sum(shared_part.astype(jnp.bfloat16), rank)

    mixer_part = mixer_finish(place[None].astype(jnp.int32), mixed, query, carried, head_gain, w_out)
    mixer_sum = scatter_sum(mixer_part, rank)
    return (mixer_sum.astype(jnp.bfloat16), (routed + shared_sum).astype(jnp.bfloat16))


def solution(mesh):
    return jax.shard_map(
        local,
        mesh=mesh,
        in_specs=(
            P("ep", None),
            P("ep"),
            P(),
            P(None, "tp"),
            P(None, "tp"),
            P(None, "tp"),
            P("tp"),
            P("tp"),
            P("tp", None),
            P("ep", None),
            P(),
            P("ep", None),
            P(("ep", "tp"), None),
            P("ep", None, "tp"),
            P("ep", None, "tp"),
            P("ep", "tp", None),
            P(None, "tp"),
            P(None, "tp"),
            P("tp", None),
        ),
        out_specs=(P(("ep", "tp"), None), P(("ep", "tp"), None)),
        check_vma=False,
    )
```

```python
import functools

import jax
import jax.numpy as jnp
from jax import lax
from jax.experimental import pallas as pl
from jax.experimental.pallas import tpu as pltpu
from jax.sharding import PartitionSpec as P

HEAD = 64
SPAN = 64

epsilon = 1e-06
route_scale = 2.5


NT = (((1,), (1,)), ((), ()))
TN = (((0,), (0,)), ((), ()))
NN = (((1,), (0,)), ((), ()))


def dot(a, b, dims=NN):
    return lax.dot_general(
        a.astype(jnp.bfloat16),
        b.astype(jnp.bfloat16),
        dims,
        preferred_element_type=jnp.float32,
    )


def two_part(x):
    high = x.astype(jnp.bfloat16)
    return high, (x - high.astype(jnp.float32)).astype(jnp.bfloat16)


def head_mask(rows, columns):
    row = lax.broadcasted_iota(jnp.int32, (rows, columns), 0) // HEAD
    column = lax.broadcasted_iota(jnp.int32, (rows, columns), 1) // HEAD
    return row == column


def norm_rows(row_data, gain_vec):
    widened = row_data.astype(jnp.float32)
    scaled = widened * lax.rsqrt(jnp.mean(widened * widened, axis=-1, keepdims=True) + epsilon)
    return (scaled * gain_vec).astype(jnp.bfloat16)


def local_scan(
    x_ref, shift_ref, gain_ref, wq_ref, wf_ref, wv_ref, room_ref,
    mixed_ref, query_ref, carry_ref, state, decay,
):
    step = pl.program_id(0)
    width = wq_ref.shape[1]
    heads = width // HEAD

    @pl.when(step == 0)
    def _():
        state[...] = jnp.zeros_like(state)
        decay[...] = jnp.ones_like(decay)

    normed = norm_rows(x_ref[...], gain_ref[...])
    queries = dot(normed, wq_ref[...])
    queries = queries / (1.0 + jnp.exp(-queries))
    before = dot(normed, wf_ref[...]) + shift_ref[...]
    values = dot(normed, wv_ref[...])
    rate = room_ref[...] / (1.0 + jnp.exp(before))
    log_forget = jnp.log1p(-rate)
    causal = (
        lax.broadcasted_iota(jnp.int32, (SPAN, SPAN), 0)
        >= lax.broadcasted_iota(jnp.int32, (SPAN, SPAN), 1)
    )
    lower = causal.astype(jnp.bfloat16)
    high, low = two_part(log_forget)
    log_decay = dot(lower, high) + dot(lower, low)
    middle = log_decay[SPAN // 2 : SPAN // 2 + 1]
    block_end = log_decay[SPAN - 1 :]
    left = (queries * jnp.exp(log_decay - middle)).astype(jnp.bfloat16)
    right = rate * jnp.exp(middle - log_decay)
    mask = head_mask(width, width)
    stacked = jnp.concatenate([left] * heads, axis=0)
    stacked = jnp.where(mask, stacked, jnp.zeros_like(stacked))
    scores = dot(stacked, right, NT)
    scores = jnp.where(jnp.concatenate([causal] * heads, axis=0), scores, 0.0)
    spread = jnp.where(mask, dot(scores, values), 0.0)
    within = spread[:SPAN]
    for head in range(1, heads):
        within = within + spread[head * SPAN : (head + 1) * SPAN]
    query_decay = queries * jnp.exp(log_decay)
    mixed_ref[...] = within + dot(query_decay, state[...], NT)
    query_ref[...] = (query_decay * decay[...]).astype(jnp.bfloat16)
    added = dot(values, rate * jnp.exp(block_end - log_decay), TN)
    total = jnp.exp(block_end)
    new_state = total * state[...] + jnp.where(mask, added, 0.0)
    state[...] = new_state
    decay[...] = decay[...] * total

    @pl.when(step == pl.num_programs(0) - 1)
    def _():
        packed = new_state[:HEAD]
        for head in range(1, heads):
            packed = packed + new_state[head * HEAD : (head + 1) * HEAD]
        high, low = two_part(decay[...])
        row = lax.broadcasted_iota(jnp.int32, (16, width), 0)
        tail = jnp.where(row == 0, high.astype(jnp.float32), 0.0)
        tail = jnp.where(row == 1, low.astype(jnp.float32), tail)
        carry_ref[:HEAD] = packed.astype(jnp.bfloat16)
        carry_ref[HEAD:] = tail.astype(jnp.bfloat16)


def finish(mixed_ref, query_ref, all_ref, gain_ref, out_w_ref, part_ref, start):
    width = mixed_ref.shape[1]
    heads = width // HEAD
    mask = head_mask(width, width)

    @pl.when(pl.program_id(0) == 0)
    def _():
        def one(lap, state):
            block = all_ref[lap].astype(jnp.float32)
            total = block[HEAD : HEAD + 1] + block[HEAD + 1 : HEAD + 2]
            return total * state + block[:HEAD]

        packed = lax.fori_loop(
            0, all_ref.shape[0], one, jnp.zeros((HEAD, width), jnp.float32)
        )
        whole = jnp.concatenate([packed] * heads, axis=0)
        start[...] = jnp.where(mask, whole, 0.0).astype(jnp.bfloat16)

    mixed = mixed_ref[...] + dot(query_ref[...], start[...], NT)
    ones = mask.astype(jnp.bfloat16)
    high, low = two_part(mixed * mixed)
    square = (dot(high, ones) + dot(low, ones)) * (1.0 / HEAD)
    head_out = (mixed * lax.rsqrt(square + epsilon) * gain_ref[...]).astype(jnp.bfloat16)
    part_ref[...] = dot(head_out, out_w_ref[...]).astype(jnp.bfloat16)


def whole_block(array):
    return pl.BlockSpec(array.shape, lambda i, rank=array.ndim: (0,) * rank)


def mixer_scan(mix_in, forget_shift, mix_gain, w_query, w_forget, w_value, forget_room):
    rows, width = mix_in.shape[0], w_query.shape[1]
    gain = mix_gain[None]
    room = forget_room[None]
    by_span = lambda columns: pl.BlockSpec((SPAN, columns), lambda i: (i, 0))
    return pl.pallas_call(
        local_scan,
        grid=(rows // SPAN,),
        in_specs=[
            by_span(mix_in.shape[1]), by_span(1), whole_block(gain), whole_block(w_query),
            whole_block(w_forget), whole_block(w_value), whole_block(room),
        ],
        out_specs=[
            by_span(width), by_span(width),
            pl.BlockSpec((HEAD + 16, width), lambda i: (0, 0)),
        ],
        out_shape=[
            jax.ShapeDtypeStruct((rows, width), jnp.float32),
            jax.ShapeDtypeStruct((rows, width), jnp.bfloat16),
            jax.ShapeDtypeStruct((HEAD + 16, width), jnp.bfloat16),
        ],
        scratch_shapes=[
            pltpu.VMEM((width, width), jnp.float32),
            pltpu.VMEM((1, width), jnp.float32),
        ],
        compiler_params=pltpu.CompilerParams(vmem_limit_bytes=32 * 1024 * 1024),
        cost_estimate=pl.CostEstimate(
            flops=40_000_000_000 * rows // 512, bytes_accessed=7_000_000, transcendentals=0
        ),
        name="mixer_scan",
    )(mix_in, forget_shift[:, None], gain, w_query, w_forget, w_value, room)


def mixer_finish(mixed, query, carried, head_gain, w_out):
    rows, width = mixed.shape
    block = min(rows, 4 * SPAN)
    gain = head_gain[None]
    by_rows = lambda columns: pl.BlockSpec((block, columns), lambda i: (i, 0))
    return pl.pallas_call(
        finish,
        grid=(rows // block,),
        in_specs=[
            by_rows(width), by_rows(width),
            whole_block(carried), whole_block(gain), whole_block(w_out),
        ],
        out_specs=by_rows(w_out.shape[1]),
        out_shape=jax.ShapeDtypeStruct((rows, w_out.shape[1]), jnp.bfloat16),
        scratch_shapes=[pltpu.VMEM((width, width), jnp.bfloat16)],
        compiler_params=pltpu.CompilerParams(vmem_limit_bytes=32 * 1024 * 1024),
        cost_estimate=pl.CostEstimate(
            flops=4_000_000_000, bytes_accessed=5_000_000, transcendentals=0
        ),
        name="mixer_finish",
    )(mixed, query, carried, gain, w_out)


def swap(x, axis, bit):
    return lax.ppermute(x, axis, [(i, i ^ bit) for i in range(lax.axis_size(axis))])


def axis_bits(axis):
    return [1 << i for i in range(lax.axis_size(axis).bit_length() - 1)]


def split_bits(part, axis):
    bits = axis_bits(axis)
    rows = part.shape[0] >> len(bits)
    return part.reshape((2,) * len(bits) + (rows, part.shape[1])), bits[::-1]


def halve(held, axis, bit):
    part, bits = held
    part = part.astype(jnp.bfloat16)
    at = bits.index(bit)
    mine = (lax.axis_index(axis) // bit) % 2
    keep = lax.dynamic_index_in_dim(part, mine, at, False)
    send = lax.dynamic_index_in_dim(part, 1 - mine, at, False)
    total = keep.astype(jnp.float32) + swap(send, axis, bit).astype(jnp.float32)
    return total, [b for b in bits if b != bit]


def halve_all(held, axis, order):
    for bit in order:
        held = halve(held, axis, bit)
    return held[0]


def gather_groups(w):
    bits = axis_bits("tp")
    near, far = bits[0], bits[1:]
    away = []
    for bit in far[::-1]:
        away = away + [swap(x, "tp", bit) for x in [w] + away]
    home = [w, swap(w, "tp", near)]
    return home, [y for x in away for y in (x, swap(x, "tp", near))]


def carried_blocks(carry):
    count = lax.axis_size("ep")
    if count > 8:
        held = lax.all_gather(carry, "ep")
        before = jnp.arange(count)[:, None, None] < lax.axis_index("ep")
        return jnp.where(before, held, jnp.zeros_like(held))
    return jnp.stack(
        [
            lax.ppermute(carry, "ep", [(i, i + d) for i in range(count - d)])
            for d in range(count - 1, 0, -1)
        ]
    )


def hidden_units(rows_ref, *refs):
    count = (len(refs) - 1) // 2
    act_ref = refs[-1]
    rows = rows_ref[...]
    width = refs[0].shape[1]
    for group in range(count):
        gate = dot(rows, refs[group][...])
        up = dot(rows, refs[count + group][...])
        act = gate / (1.0 + jnp.exp(-gate)) * up
        act_ref[:, group * width : (group + 1) * width] = act.astype(jnp.bfloat16)


def expert_units(gathered, gates, ups):
    rows, model, width = gathered.shape[0], gates[0].shape[0], gates[0].shape[1]
    block = min(rows, 256)
    count = len(gates)
    return pl.pallas_call(
        hidden_units,
        grid=(rows // block,),
        in_specs=[pl.BlockSpec((block, model), lambda i: (i, 0))]
        + [whole_block(w) for w in gates + ups],
        out_specs=pl.BlockSpec((block, count * width), lambda i: (i, 0)),
        out_shape=jax.ShapeDtypeStruct((rows, count * width), jnp.bfloat16),
        compiler_params=pltpu.CompilerParams(vmem_limit_bytes=40 * 1024 * 1024),
        cost_estimate=pl.CostEstimate(
            flops=4 * rows * model * width * count,
            bytes_accessed=2 * (2 * count * model * width + rows * model),
            transcendentals=0,
        ),
        name="expert_units",
    )(gathered, *gates, *ups)


def weighted_rows(experts, place_ref, share_ref, *refs):
    out_ref = refs[-1]
    acts = jnp.concatenate([ref[...] for ref in refs[:2]], axis=1)
    downs = refs[2:-1]
    width = downs[0].shape[0]
    result = dot(acts[:, :width], downs[0][...])
    for group in range(1, len(downs)):
        result = result + dot(acts[:, group * width : (group + 1) * width], downs[group][...])
    lane = lax.broadcasted_iota(jnp.int32, share_ref.shape, 1)
    chosen = (lane == place_ref[0]) | (lane == place_ref[0] + experts)
    share = jnp.sum(
        jnp.where(chosen, share_ref[...].astype(jnp.float32), 0.0), axis=1, keepdims=True
    )
    out_ref[...] = (result * share).astype(jnp.bfloat16)


def expert_rows(place, gathered, model, experts, acts, downs):
    rows, columns = gathered.shape[0], downs[0].shape[1]
    spare = gathered.shape[1] - model
    block = min(rows, 256)
    return pl.pallas_call(
        functools.partial(weighted_rows, experts),
        grid=(rows // block,),
        in_specs=[
            pl.BlockSpec(memory_space=pltpu.SMEM),
            pl.BlockSpec((block, spare), lambda i: (i, model // spare)),
        ]
        + [pl.BlockSpec((block, act.shape[1]), lambda i: (i, 0)) for act in acts]
        + [whole_block(w) for w in downs],
        out_specs=pl.BlockSpec((block, columns), lambda i: (i, 0)),
        out_shape=jax.ShapeDtypeStruct((rows, columns), jnp.bfloat16),
        compiler_params=pltpu.CompilerParams(vmem_limit_bytes=40 * 1024 * 1024),
        cost_estimate=pl.CostEstimate(
            flops=2 * rows * columns * (acts[0].shape[1] + acts[1].shape[1]),
            bytes_accessed=8_000_000,
            transcendentals=0,
        ),
        name="expert_rows",
    )(place, gathered, *acts, *downs)


def local(
    mix_in, forget_shift, mix_gain, w_query, w_forget, w_value, forget_room, head_gain, w_out,
    moe_in, moe_gain, expert_choice, route_logit, w_exp_gate, w_exp_up, w_exp_down,
    w_sh_gate, w_sh_up, w_sh_down,
):
    tp_count = lax.axis_size("tp")
    rank = lax.axis_index("tp")
    place = lax.axis_index("ep")
    experts = lax.axis_size("ep") * w_exp_gate.shape[0]
    quarter = moe_in.shape[0] // tp_count
    model = moe_in.shape[1]

    half = model // 2
    flat = lambda w: w.reshape(w.shape[1:])
    gates, far_gates = gather_groups(flat(w_exp_gate))
    ups, far_ups = gather_groups(flat(w_exp_up))
    left_downs = sum(gather_groups(flat(w_exp_down)[:, :half]), [])
    right_downs = sum(gather_groups(flat(w_exp_down)[:, half:]), [])

    hidden = norm_rows(moe_in, moe_gain)
    chance = jax.nn.sigmoid(route_logit)
    weights = chance / jnp.sum(chance, axis=-1, keepdims=True) * route_scale
    own_choice = lax.dynamic_slice_in_dim(expert_choice, rank * quarter, quarter, 0)
    table = jnp.sum(
        jnp.where(
            own_choice[..., None] == jnp.arange(experts, dtype=jnp.int32),
            weights[..., None],
            0.0,
        ),
        axis=1,
    )
    high, low = two_part(table)
    spare = -(2 * experts) % 128
    own_rows = lax.dynamic_slice_in_dim(hidden, rank * quarter, quarter, 0)
    sent = jnp.concatenate(
        [own_rows, high, low, jnp.zeros((quarter, spare), jnp.bfloat16)], axis=1
    )
    gathered = lax.all_gather(sent, "ep", axis=0, tiled=True)

    mixed, query, carry = mixer_scan(
        mix_in, forget_shift, mix_gain, w_query, w_forget, w_value, forget_room
    )
    mixer_part = mixer_finish(mixed, query, carried_blocks(carry), head_gain, w_out)
    shared_gate = jnp.dot(hidden, w_sh_gate, preferred_element_type=jnp.float32)
    shared_up = jnp.dot(hidden, w_sh_up, preferred_element_type=jnp.float32)
    shared_act = (jax.nn.silu(shared_gate) * shared_up).astype(jnp.bfloat16)
    shared_part = jnp.dot(shared_act, w_sh_down, preferred_element_type=jnp.float32)
    tp_bits = axis_bits("tp")
    mixer_held, mixer_bits = halve(split_bits(mixer_part, "tp"), "tp", tp_bits[0])
    shared_held, shared_bits = halve(split_bits(shared_part, "tp"), "tp", tp_bits[0])
    mixer_held, shared_held = mixer_held.astype(jnp.bfloat16), shared_held.astype(jnp.bfloat16)

    gathered, mixer_held, shared_held = lax.optimization_barrier(
        (gathered, mixer_held, shared_held)
    )
    acts = [expert_units(gathered, gates, ups), expert_units(gathered, far_gates, far_ups)]
    spot = place[None].astype(jnp.int32)
    left = expert_rows(spot, gathered, model, experts, acts, left_downs)
    right = expert_rows(spot, gathered, model, experts, acts, right_downs)

    right, mixer_held, shared_held = lax.optimization_barrier((right, mixer_held, shared_held))
    ep_bits = axis_bits("ep")
    left = halve_all(split_bits(left, "ep"), "ep", ep_bits)
    right = halve_all(split_bits(right, "ep"), "ep", ep_bits[1:] + ep_bits[:1])
    mixer_sum = halve_all((mixer_held, mixer_bits), "tp", tp_bits[1:])
    shared_sum = halve_all((shared_held, shared_bits), "tp", tp_bits[1:])
    routed = jnp.concatenate([left, right], axis=1)
    return (mixer_sum.astype(jnp.bfloat16), (routed + shared_sum).astype(jnp.bfloat16))


def solution(mesh):
    return jax.shard_map(
        local,
        mesh=mesh,
        in_specs=(
            P("ep", None),
            P("ep"),
            P(),
            P(None, "tp"),
            P(None, "tp"),
            P(None, "tp"),
            P("tp"),
            P("tp"),
            P("tp", None),
            P("ep", None),
            P(),
            P("ep", None),
            P(("ep", "tp"), None),
            P("ep", None, "tp"),
            P("ep", None, "tp"),
            P("ep", "tp", None),
            P(None, "tp"),
            P(None, "tp"),
            P("tp", None),
        ),
        out_specs=(P(("ep", "tp"), None), P(("ep", "tp"), None)),
        check_vma=False,
    )
```

```python
import functools

import jax
import jax.numpy as jnp
from jax import lax
from jax.experimental import pallas as pl
from jax.experimental.pallas import tpu as pltpu
from jax.sharding import PartitionSpec as P


HEAD = 64
SPAN = 64

epsilon = 1e-06
route_scale = 2.5


NT = (((1,), (1,)), ((), ()))
TN = (((0,), (0,)), ((), ()))
NN = (((1,), (0,)), ((), ()))


def dot(a, b, dims=NN):
    return lax.dot_general(
        a.astype(jnp.bfloat16),
        b.astype(jnp.bfloat16),
        dims,
        preferred_element_type=jnp.float32,
    )


def two_part(x):
    high = x.astype(jnp.bfloat16)
    return high, (x - high.astype(jnp.float32)).astype(jnp.bfloat16)


def head_mask(rows, columns):
    row = lax.broadcasted_iota(jnp.int32, (rows, columns), 0) // HEAD
    column = lax.broadcasted_iota(jnp.int32, (rows, columns), 1) // HEAD
    return row == column


def norm_rows(row_data, gain_vec):
    widened = row_data.astype(jnp.float32)
    scaled = widened * lax.rsqrt(jnp.mean(widened * widened, axis=-1, keepdims=True) + epsilon)
    return (scaled * gain_vec).astype(jnp.bfloat16)


def local_scan(
    x_ref, shift_ref, gain_ref, wq_ref, wf_ref, wv_ref, room_ref,
    mixed_ref, query_ref, carry_ref, state, decay,
):
    step = pl.program_id(0)
    width = wq_ref.shape[1]
    heads = width // HEAD

    @pl.when(step == 0)
    def _():
        state[...] = jnp.zeros_like(state)
        decay[...] = jnp.ones_like(decay)

    normed = norm_rows(x_ref[...], gain_ref[...])
    queries = dot(normed, wq_ref[...])
    queries = queries / (1.0 + jnp.exp(-queries))
    before = dot(normed, wf_ref[...]) + shift_ref[...]
    values = dot(normed, wv_ref[...])
    rate = room_ref[...] / (1.0 + jnp.exp(before))
    log_forget = jnp.log1p(-rate)
    causal = (
        lax.broadcasted_iota(jnp.int32, (SPAN, SPAN), 0)
        >= lax.broadcasted_iota(jnp.int32, (SPAN, SPAN), 1)
    )
    lower = causal.astype(jnp.bfloat16)
    high, low = two_part(log_forget)
    log_decay = dot(lower, high) + dot(lower, low)
    middle = log_decay[SPAN // 2 : SPAN // 2 + 1]
    block_end = log_decay[SPAN - 1 :]
    left = (queries * jnp.exp(log_decay - middle)).astype(jnp.bfloat16)
    right = rate * jnp.exp(middle - log_decay)
    mask = head_mask(width, width)
    stacked = jnp.concatenate([left] * heads, axis=0)
    stacked = jnp.where(mask, stacked, jnp.zeros_like(stacked))
    scores = dot(stacked, right, NT)
    scores = jnp.where(jnp.concatenate([causal] * heads, axis=0), scores, 0.0)
    spread = jnp.where(mask, dot(scores, values), 0.0)
    within = spread[:SPAN]
    for head in range(1, heads):
        within = within + spread[head * SPAN : (head + 1) * SPAN]
    query_decay = queries * jnp.exp(log_decay)
    mixed_ref[...] = within + dot(query_decay, state[...], NT)
    query_ref[...] = (query_decay * decay[...]).astype(jnp.bfloat16)
    added = dot(values, rate * jnp.exp(block_end - log_decay), TN)
    total = jnp.exp(block_end)
    new_state = total * state[...] + jnp.where(mask, added, 0.0)
    state[...] = new_state
    decay[...] = decay[...] * total

    @pl.when(step == pl.num_programs(0) - 1)
    def _():
        packed = new_state[:HEAD]
        for head in range(1, heads):
            packed = packed + new_state[head * HEAD : (head + 1) * HEAD]
        high, low = two_part(decay[...])
        row = lax.broadcasted_iota(jnp.int32, (16, width), 0)
        tail = jnp.where(row == 0, high.astype(jnp.float32), 0.0)
        tail = jnp.where(row == 1, low.astype(jnp.float32), tail)
        carry_ref[:HEAD] = packed.astype(jnp.bfloat16)
        carry_ref[HEAD:] = tail.astype(jnp.bfloat16)


def finish(mixed_ref, query_ref, all_ref, gain_ref, out_w_ref, part_ref, start):
    width = mixed_ref.shape[1]
    heads = width // HEAD
    mask = head_mask(width, width)

    @pl.when(pl.program_id(0) == 0)
    def _():
        def one(lap, state):
            block = all_ref[lap].astype(jnp.float32)
            total = block[HEAD : HEAD + 1] + block[HEAD + 1 : HEAD + 2]
            return total * state + block[:HEAD]

        packed = lax.fori_loop(
            0, all_ref.shape[0], one, jnp.zeros((HEAD, width), jnp.float32)
        )
        whole = jnp.concatenate([packed] * heads, axis=0)
        start[...] = jnp.where(mask, whole, 0.0).astype(jnp.bfloat16)

    mixed = mixed_ref[...] + dot(query_ref[...], start[...], NT)
    ones = mask.astype(jnp.bfloat16)
    high, low = two_part(mixed * mixed)
    square = (dot(high, ones) + dot(low, ones)) * (1.0 / HEAD)
    head_out = (mixed * lax.rsqrt(square + epsilon) * gain_ref[...]).astype(jnp.bfloat16)
    part_ref[...] = dot(head_out, out_w_ref[...]).astype(jnp.bfloat16)


def whole_block(array):
    return pl.BlockSpec(array.shape, lambda i, rank=array.ndim: (0,) * rank)


def mixer_scan(mix_in, forget_shift, mix_gain, w_query, w_forget, w_value, forget_room):
    rows, width = mix_in.shape[0], w_query.shape[1]
    gain = mix_gain[None]
    room = forget_room[None]
    by_span = lambda columns: pl.BlockSpec((SPAN, columns), lambda i: (i, 0))
    return pl.pallas_call(
        local_scan,
        grid=(rows // SPAN,),
        in_specs=[
            by_span(mix_in.shape[1]), by_span(1), whole_block(gain), whole_block(w_query),
            whole_block(w_forget), whole_block(w_value), whole_block(room),
        ],
        out_specs=[
            by_span(width), by_span(width),
            pl.BlockSpec((HEAD + 16, width), lambda i: (0, 0)),
        ],
        out_shape=[
            jax.ShapeDtypeStruct((rows, width), jnp.float32),
            jax.ShapeDtypeStruct((rows, width), jnp.bfloat16),
            jax.ShapeDtypeStruct((HEAD + 16, width), jnp.bfloat16),
        ],
        scratch_shapes=[
            pltpu.VMEM((width, width), jnp.float32),
            pltpu.VMEM((1, width), jnp.float32),
        ],
        compiler_params=pltpu.CompilerParams(vmem_limit_bytes=32 * 1024 * 1024),
        cost_estimate=pl.CostEstimate(
            flops=40_000_000_000 * rows // 512, bytes_accessed=7_000_000, transcendentals=0
        ),
        name="mixer_scan",
    )(mix_in, forget_shift[:, None], gain, w_query, w_forget, w_value, room)


def mixer_finish(mixed, query, carried, head_gain, w_out):
    rows, width = mixed.shape
    block = min(rows, 4 * SPAN)
    gain = head_gain[None]
    by_rows = lambda columns: pl.BlockSpec((block, columns), lambda i: (i, 0))
    return pl.pallas_call(
        finish,
        grid=(rows // block,),
        in_specs=[
            by_rows(width), by_rows(width),
            whole_block(carried), whole_block(gain), whole_block(w_out),
        ],
        out_specs=by_rows(w_out.shape[1]),
        out_shape=jax.ShapeDtypeStruct((rows, w_out.shape[1]), jnp.bfloat16),
        scratch_shapes=[pltpu.VMEM((width, width), jnp.bfloat16)],
        compiler_params=pltpu.CompilerParams(vmem_limit_bytes=32 * 1024 * 1024),
        cost_estimate=pl.CostEstimate(
            flops=4_000_000_000, bytes_accessed=5_000_000, transcendentals=0
        ),
        name="mixer_finish",
    )(mixed, query, carried, gain, w_out)


def swap(x, axis, bit):
    return lax.ppermute(x, axis, [(i, i ^ bit) for i in range(lax.axis_size(axis))])


def axis_bits(axis):
    return [1 << i for i in range(lax.axis_size(axis).bit_length() - 1)]


def split_bits(part, axis):
    bits = axis_bits(axis)
    rows = part.shape[0] >> len(bits)
    return part.reshape((2,) * len(bits) + (rows, part.shape[1])), bits[::-1]


def halve(held, axis, bit):
    part, bits = held
    part = part.astype(jnp.bfloat16)
    at = bits.index(bit)
    mine = (lax.axis_index(axis) // bit) % 2
    keep = lax.dynamic_index_in_dim(part, mine, at, False)
    send = lax.dynamic_index_in_dim(part, 1 - mine, at, False)
    total = keep.astype(jnp.float32) + swap(send, axis, bit).astype(jnp.float32)
    return total, [b for b in bits if b != bit]


def halve_all(held, axis, order):
    for bit in order:
        held = halve(held, axis, bit)
    return held[0]


def gather_rows(x, axis, order):
    bits = []
    for bit in order:
        at = sum(b > bit for b in bits)
        x = jnp.stack([x, swap(x, axis, bit)], axis=at)
        bits = sorted(bits + [bit], reverse=True)
    return x.reshape(-1, x.shape[-1])


def scatter_rows(part, axis, order):
    bits = axis_bits(axis)[::-1]
    part = part.reshape((2,) * len(bits) + (part.shape[0] >> len(bits), part.shape[1]))
    for bit in order:
        at = bits.index(bit)
        part = part.astype(jnp.bfloat16)
        keep = lax.index_in_dim(part, 0, at, False).astype(jnp.float32)
        part = keep + swap(lax.index_in_dim(part, 1, at, False), axis, bit).astype(jnp.float32)
        bits = [b for b in bits if b != bit]
    return part


def gather_groups(w):
    bits = axis_bits("tp")
    near, far = bits[0], bits[1:]
    away = []
    for bit in far[::-1]:
        away = away + [swap(x, "tp", bit) for x in [w] + away]
    home = [w, swap(w, "tp", near)]
    return home, [y for x in away for y in (x, swap(x, "tp", near))]


def carried_blocks(carry):
    count = lax.axis_size("ep")
    if count > 8:
        held = lax.all_gather(carry, "ep")
        before = jnp.arange(count)[:, None, None] < lax.axis_index("ep")
        return jnp.where(before, held, jnp.zeros_like(held))
    return jnp.stack(
        [
            lax.ppermute(carry, "ep", [(i, i + d) for i in range(count - d)])
            for d in range(count - 1, 0, -1)
        ]
    )


def hidden_units(left_ref, right_ref, *refs):
    count = (len(refs) - 1) // 2
    act_ref = refs[-1]
    rows = jnp.concatenate([left_ref[...], right_ref[...]], axis=1)
    width = refs[0].shape[1]
    for group in range(count):
        gate = dot(rows, refs[group][...])
        up = dot(rows, refs[count + group][...])
        act = gate / (1.0 + jnp.exp(-gate)) * up
        act_ref[:, group * width : (group + 1) * width] = act.astype(jnp.bfloat16)


def expert_units(left, right, gates, ups):
    rows, model, width = left.shape[0], gates[0].shape[0], gates[0].shape[1]
    block = min(rows, 256)
    count = len(gates)
    return pl.pallas_call(
        hidden_units,
        grid=(rows // block,),
        in_specs=[pl.BlockSpec((block, model // 2), lambda i: (i, 0))] * 2
        + [whole_block(w) for w in gates + ups],
        out_specs=pl.BlockSpec((block, count * width), lambda i: (i, 0)),
        out_shape=jax.ShapeDtypeStruct((rows, count * width), jnp.bfloat16),
        compiler_params=pltpu.CompilerParams(vmem_limit_bytes=40 * 1024 * 1024),
        cost_estimate=pl.CostEstimate(
            flops=4 * rows * model * width * count,
            bytes_accessed=2 * (2 * count * model * width + rows * model),
            transcendentals=0,
        ),
        name="expert_units",
    )(left, right, *gates, *ups)


def weighted_rows(experts, place_ref, share_ref, *refs):
    out_ref = refs[-1]
    acts = jnp.concatenate([ref[...] for ref in refs[:2]], axis=1)
    downs = refs[2:-1]
    width = downs[0].shape[0]
    result = dot(acts[:, :width], downs[0][...])
    for group in range(1, len(downs)):
        result = result + dot(acts[:, group * width : (group + 1) * width], downs[group][...])
    lane = lax.broadcasted_iota(jnp.int32, share_ref.shape, 1)
    chosen = (lane == place_ref[0]) | (lane == place_ref[0] + experts)
    share = jnp.sum(
        jnp.where(chosen, share_ref[...].astype(jnp.float32), 0.0), axis=1, keepdims=True
    )
    out_ref[...] = (result * share).astype(jnp.bfloat16)


def expert_rows(place, gathered, model, experts, acts, downs):
    rows, columns = gathered.shape[0], downs[0].shape[1]
    spare = gathered.shape[1] - model
    block = min(rows, 256)
    return pl.pallas_call(
        functools.partial(weighted_rows, experts),
        grid=(rows // block,),
        in_specs=[
            pl.BlockSpec(memory_space=pltpu.SMEM),
            pl.BlockSpec((block, spare), lambda i: (i, model // spare)),
        ]
        + [pl.BlockSpec((block, act.shape[1]), lambda i: (i, 0)) for act in acts]
        + [whole_block(w) for w in downs],
        out_specs=pl.BlockSpec((block, columns), lambda i: (i, 0)),
        out_shape=jax.ShapeDtypeStruct((rows, columns), jnp.bfloat16),
        compiler_params=pltpu.CompilerParams(vmem_limit_bytes=40 * 1024 * 1024),
        cost_estimate=pl.CostEstimate(
            flops=2 * rows * columns * (acts[0].shape[1] + acts[1].shape[1]),
            bytes_accessed=8_000_000,
            transcendentals=0,
        ),
        name="expert_rows",
    )(place, gathered, *acts, *downs)


def local(
    mix_in, forget_shift, mix_gain, w_query, w_forget, w_value, forget_room, head_gain, w_out,
    moe_in, moe_gain, expert_choice, route_logit, w_exp_gate, w_exp_up, w_exp_down,
    w_sh_gate, w_sh_up, w_sh_down,
):
    tp_count = lax.axis_size("tp")
    rank = lax.axis_index("tp")
    place = lax.axis_index("ep")
    experts = lax.axis_size("ep") * w_exp_gate.shape[0]
    quarter = moe_in.shape[0] // tp_count
    model = moe_in.shape[1]

    half = model // 2
    flat = lambda w: w.reshape(w.shape[1:])
    gates, far_gates = gather_groups(flat(w_exp_gate))
    ups, far_ups = gather_groups(flat(w_exp_up))
    left_downs = sum(gather_groups(flat(w_exp_down)[:, :half]), [])
    right_downs = sum(gather_groups(flat(w_exp_down)[:, half:]), [])

    hidden = norm_rows(moe_in, moe_gain)
    chance = jax.nn.sigmoid(route_logit)
    weights = chance / jnp.sum(chance, axis=-1, keepdims=True) * route_scale
    own_choice = lax.dynamic_slice_in_dim(expert_choice, rank * quarter, quarter, 0)
    table = jnp.sum(
        jnp.where(
            own_choice[..., None] == jnp.arange(experts, dtype=jnp.int32),
            weights[..., None],
            0.0,
        ),
        axis=1,
    )
    high, low = two_part(table)
    spare = -(2 * experts) % 128
    own_rows = lax.dynamic_slice_in_dim(hidden, rank * quarter, quarter, 0)
    sent = jnp.concatenate(
        [own_rows[:, half:], high, low, jnp.zeros((quarter, spare), jnp.bfloat16)], axis=1
    )
    ep_bits = axis_bits("ep")
    turned = ep_bits[1:] + ep_bits[:1]
    left_rows = gather_rows(own_rows[:, :half], "ep", ep_bits)
    right_rows = gather_rows(sent, "ep", turned)

    mixed, query, carry = mixer_scan(
        mix_in, forget_shift, mix_gain, w_query, w_forget, w_value, forget_room
    )
    mixer_part = mixer_finish(mixed, query, carried_blocks(carry), head_gain, w_out)
    shared_gate = jnp.dot(hidden, w_sh_gate, preferred_element_type=jnp.float32)
    shared_up = jnp.dot(hidden, w_sh_up, preferred_element_type=jnp.float32)
    shared_act = (jax.nn.silu(shared_gate) * shared_up).astype(jnp.bfloat16)
    shared_part = jnp.dot(shared_act, w_sh_down, preferred_element_type=jnp.float32)
    tp_bits = axis_bits("tp")
    mixer_held, mixer_bits = halve(split_bits(mixer_part, "tp"), "tp", tp_bits[0])
    shared_held, shared_bits = halve(split_bits(shared_part, "tp"), "tp", tp_bits[0])
    mixer_held, shared_held = mixer_held.astype(jnp.bfloat16), shared_held.astype(jnp.bfloat16)

    left_rows, right_rows, mixer_held, shared_held = lax.optimization_barrier(
        (left_rows, right_rows, mixer_held, shared_held)
    )
    home_act = expert_units(left_rows, right_rows, gates, ups)
    away_act = expert_units(left_rows, right_rows, far_gates, far_ups)
    acts = [home_act, away_act]
    spot = place[None].astype(jnp.int32)
    left = expert_rows(spot, right_rows, half, experts, acts, left_downs)
    right = expert_rows(spot, right_rows, half, experts, acts, right_downs)

    right, mixer_held, shared_held = lax.optimization_barrier((right, mixer_held, shared_held))
    left = scatter_rows(left, "ep", ep_bits)
    right = scatter_rows(right, "ep", turned)
    mixer_sum = halve_all((mixer_held, mixer_bits), "tp", tp_bits[1:])
    shared_sum = halve_all((shared_held, shared_bits), "tp", tp_bits[1:])
    routed = jnp.concatenate([left, right], axis=1)
    return (mixer_sum.astype(jnp.bfloat16), (routed + shared_sum).astype(jnp.bfloat16))


def solution(mesh):
    return jax.shard_map(
        local,
        mesh=mesh,
        in_specs=(
            P("ep", None),
            P("ep"),
            P(),
            P(None, "tp"),
            P(None, "tp"),
            P(None, "tp"),
            P("tp"),
            P("tp"),
            P("tp", None),
            P("ep", None),
            P(),
            P("ep", None),
            P(("ep", "tp"), None),
            P("ep", None, "tp"),
            P("ep", None, "tp"),
            P("ep", "tp", None),
            P(None, "tp"),
            P(None, "tp"),
            P("tp", None),
        ),
        out_specs=(P(("ep", "tp"), None), P(("ep", "tp"), None)),
        check_vma=False,
    )
```

```python
import functools

import jax
import jax.numpy as jnp
from jax import lax
from jax.experimental import pallas as pl
from jax.experimental.pallas import tpu as pltpu
from jax.sharding import PartitionSpec as P


HEAD = 64
SPAN = 64

epsilon = 1e-06
route_scale = 2.5


NT = (((1,), (1,)), ((), ()))
TN = (((0,), (0,)), ((), ()))
NN = (((1,), (0,)), ((), ()))


def dot(a, b, dims=NN):
    return lax.dot_general(
        a.astype(jnp.bfloat16),
        b.astype(jnp.bfloat16),
        dims,
        preferred_element_type=jnp.float32,
    )


def two_part(x):
    high = x.astype(jnp.bfloat16)
    return high, (x - high.astype(jnp.float32)).astype(jnp.bfloat16)


def head_mask(rows, columns):
    row = lax.broadcasted_iota(jnp.int32, (rows, columns), 0) // HEAD
    column = lax.broadcasted_iota(jnp.int32, (rows, columns), 1) // HEAD
    return row == column


def norm_rows(row_data, gain_vec):
    widened = row_data.astype(jnp.float32)
    scaled = widened * lax.rsqrt(jnp.mean(widened * widened, axis=-1, keepdims=True) + epsilon)
    return (scaled * gain_vec).astype(jnp.bfloat16)


def local_scan(
    x_ref, shift_ref, gain_ref, wq_ref, wf_ref, wv_ref, room_ref,
    mixed_ref, query_ref, carry_ref, state, decay,
):
    step = pl.program_id(0)
    width = wq_ref.shape[1]
    heads = width // HEAD

    @pl.when(step == 0)
    def _():
        state[...] = jnp.zeros_like(state)
        decay[...] = jnp.ones_like(decay)

    normed = norm_rows(x_ref[...], gain_ref[...])
    queries = dot(normed, wq_ref[...])
    queries = queries / (1.0 + jnp.exp(-queries))
    before = dot(normed, wf_ref[...]) + shift_ref[...]
    values = dot(normed, wv_ref[...])
    rate = room_ref[...] / (1.0 + jnp.exp(before))
    log_forget = jnp.log1p(-rate)
    causal = (
        lax.broadcasted_iota(jnp.int32, (SPAN, SPAN), 0)
        >= lax.broadcasted_iota(jnp.int32, (SPAN, SPAN), 1)
    )
    lower = causal.astype(jnp.bfloat16)
    high, low = two_part(log_forget)
    log_decay = dot(lower, high) + dot(lower, low)
    middle = log_decay[SPAN // 2 : SPAN // 2 + 1]
    block_end = log_decay[SPAN - 1 :]
    left = (queries * jnp.exp(log_decay - middle)).astype(jnp.bfloat16)
    right = rate * jnp.exp(middle - log_decay)
    mask = head_mask(width, width)
    stacked = jnp.concatenate([left] * heads, axis=0)
    stacked = jnp.where(mask, stacked, jnp.zeros_like(stacked))
    scores = dot(stacked, right, NT)
    scores = jnp.where(jnp.concatenate([causal] * heads, axis=0), scores, 0.0)
    spread = jnp.where(mask, dot(scores, values), 0.0)
    within = spread[:SPAN]
    for head in range(1, heads):
        within = within + spread[head * SPAN : (head + 1) * SPAN]
    query_decay = queries * jnp.exp(log_decay)
    mixed_ref[...] = within + dot(query_decay, state[...], NT)
    query_ref[...] = (query_decay * decay[...]).astype(jnp.bfloat16)
    added = dot(values, rate * jnp.exp(block_end - log_decay), TN)
    total = jnp.exp(block_end)
    new_state = total * state[...] + jnp.where(mask, added, 0.0)
    state[...] = new_state
    decay[...] = decay[...] * total

    @pl.when(step == pl.num_programs(0) - 1)
    def _():
        packed = new_state[:HEAD]
        for head in range(1, heads):
            packed = packed + new_state[head * HEAD : (head + 1) * HEAD]
        high, low = two_part(decay[...])
        row = lax.broadcasted_iota(jnp.int32, (16, width), 0)
        tail = jnp.where(row == 0, high.astype(jnp.float32), 0.0)
        tail = jnp.where(row == 1, low.astype(jnp.float32), tail)
        carry_ref[:HEAD] = packed.astype(jnp.bfloat16)
        carry_ref[HEAD:] = tail.astype(jnp.bfloat16)


def finish(mixed_ref, query_ref, gain_ref, out_w_ref, *refs):
    part_ref, start = refs[-2:]
    width = mixed_ref.shape[1]
    heads = width // HEAD
    mask = head_mask(width, width)

    @pl.when(pl.program_id(0) == 0)
    def _():
        def one(ref, lap, state):
            block = ref[lap].astype(jnp.float32)
            total = block[HEAD : HEAD + 1] + block[HEAD + 1 : HEAD + 2]
            return total * state + block[:HEAD]

        packed = jnp.zeros((HEAD, width), jnp.float32)
        for ref in refs[:-2]:
            packed = lax.fori_loop(0, ref.shape[0], functools.partial(one, ref), packed)
        whole = jnp.concatenate([packed] * heads, axis=0)
        start[...] = jnp.where(mask, whole, 0.0).astype(jnp.bfloat16)

    mixed = mixed_ref[...] + dot(query_ref[...], start[...], NT)
    ones = mask.astype(jnp.bfloat16)
    high, low = two_part(mixed * mixed)
    square = (dot(high, ones) + dot(low, ones)) * (1.0 / HEAD)
    head_out = (mixed * lax.rsqrt(square + epsilon) * gain_ref[...]).astype(jnp.bfloat16)
    part_ref[...] = dot(head_out, out_w_ref[...]).astype(jnp.bfloat16)


def whole_block(array):
    return pl.BlockSpec(array.shape, lambda i, rank=array.ndim: (0,) * rank)


def mixer_scan(mix_in, forget_shift, mix_gain, w_query, w_forget, w_value, forget_room):
    rows, width = mix_in.shape[0], w_query.shape[1]
    gain = mix_gain[None]
    room = forget_room[None]
    by_span = lambda columns: pl.BlockSpec((SPAN, columns), lambda i: (i, 0))
    return pl.pallas_call(
        local_scan,
        grid=(rows // SPAN,),
        in_specs=[
            by_span(mix_in.shape[1]), by_span(1), whole_block(gain), whole_block(w_query),
            whole_block(w_forget), whole_block(w_value), whole_block(room),
        ],
        out_specs=[
            by_span(width), by_span(width),
            pl.BlockSpec((HEAD + 16, width), lambda i: (0, 0)),
        ],
        out_shape=[
            jax.ShapeDtypeStruct((rows, width), jnp.float32),
            jax.ShapeDtypeStruct((rows, width), jnp.bfloat16),
            jax.ShapeDtypeStruct((HEAD + 16, width), jnp.bfloat16),
        ],
        scratch_shapes=[
            pltpu.VMEM((width, width), jnp.float32),
            pltpu.VMEM((1, width), jnp.float32),
        ],
        compiler_params=pltpu.CompilerParams(vmem_limit_bytes=32 * 1024 * 1024),
        cost_estimate=pl.CostEstimate(
            flops=40_000_000_000 * rows // 512, bytes_accessed=7_000_000, transcendentals=0
        ),
        name="mixer_scan",
    )(mix_in, forget_shift[:, None], gain, w_query, w_forget, w_value, room)


def mixer_finish(mixed, query, carried, head_gain, w_out):
    rows, width = mixed.shape
    block = min(rows, 4 * SPAN)
    gain = head_gain[None]
    by_rows = lambda columns: pl.BlockSpec((block, columns), lambda i: (i, 0))
    return pl.pallas_call(
        finish,
        grid=(rows // block,),
        in_specs=[
            by_rows(width), by_rows(width),
            whole_block(gain), whole_block(w_out),
        ] + [whole_block(c) for c in carried],
        out_specs=by_rows(w_out.shape[1]),
        out_shape=jax.ShapeDtypeStruct((rows, w_out.shape[1]), jnp.bfloat16),
        scratch_shapes=[pltpu.VMEM((width, width), jnp.bfloat16)],
        compiler_params=pltpu.CompilerParams(vmem_limit_bytes=32 * 1024 * 1024),
        cost_estimate=pl.CostEstimate(
            flops=4_000_000_000, bytes_accessed=5_000_000, transcendentals=0
        ),
        name="mixer_finish",
    )(mixed, query, gain, w_out, *carried)


def swap(x, axis, bit):
    return lax.ppermute(x, axis, [(i, i ^ bit) for i in range(lax.axis_size(axis))])


def axis_bits(axis):
    return [1 << i for i in range(lax.axis_size(axis).bit_length() - 1)]


def split_bits(part, axis):
    bits = axis_bits(axis)
    rows = part.shape[0] >> len(bits)
    return part.reshape((2,) * len(bits) + (rows, part.shape[1])), bits[::-1]


def halve(held, axis, bit):
    part, bits = held
    part = part.astype(jnp.bfloat16)
    at = bits.index(bit)
    mine = (lax.axis_index(axis) // bit) % 2
    keep = lax.dynamic_index_in_dim(part, mine, at, False)
    send = lax.dynamic_index_in_dim(part, 1 - mine, at, False)
    total = keep.astype(jnp.float32) + swap(send, axis, bit).astype(jnp.float32)
    return total, [b for b in bits if b != bit]


def halve_all(held, axis, order):
    for bit in order:
        held = halve(held, axis, bit)
    return held[0]


def gather_rows(x, axis, order):
    bits = []
    for bit in order:
        at = sum(b > bit for b in bits)
        other = swap(x, axis, bit)
        x = jnp.stack([x, other], axis=at)
        bits = sorted(bits + [bit], reverse=True)
    return x.reshape(-1, x.shape[-1])


def scatter_rows(part, axis, order):
    bits = axis_bits(axis)[::-1]
    part = part.reshape((2,) * len(bits) + (part.shape[0] >> len(bits), part.shape[1]))
    for bit in order:
        at = bits.index(bit)
        part = part.astype(jnp.bfloat16)
        keep = lax.index_in_dim(part, 0, at, False).astype(jnp.float32)
        send = lax.index_in_dim(part, 1, at, False)
        other = swap(send, axis, bit)
        part = keep + other.astype(jnp.float32)
        bits = [b for b in bits if b != bit]
    return part


def gather_groups(w):
    bits = axis_bits("tp")
    near, far = bits[0], bits[1:]
    away = []
    for bit in far[::-1]:
        away = away + [swap(x, "tp", bit) for x in [w] + away]
    home = [w, swap(w, "tp", near)]
    return home, [y for x in away for y in (x, swap(x, "tp", near))]


def carried_blocks(carry):
    count = lax.axis_size("ep")
    if count > 8:
        held = lax.all_gather(carry, "ep")
        before = jnp.arange(count)[:, None, None] < lax.axis_index("ep")
        return [jnp.where(before, held, jnp.zeros_like(held))]
    return [
        lax.ppermute(carry, "ep", [(i, i + d) for i in range(count - d)])[None]
        for d in range(count - 1, 0, -1)
    ]


def hidden_units(left_ref, right_ref, *refs):
    count = (len(refs) - 1) // 2
    act_ref = refs[-1]
    rows = jnp.concatenate([left_ref[...], right_ref[...]], axis=1)
    width = refs[0].shape[1]
    for group in range(count):
        gate = dot(rows, refs[group][...])
        up = dot(rows, refs[count + group][...])
        act = gate / (1.0 + jnp.exp(-gate)) * up
        act_ref[:, group * width : (group + 1) * width] = act.astype(jnp.bfloat16)


def expert_units(left, right, gates, ups):
    rows, model, width = left.shape[0], gates[0].shape[0], gates[0].shape[1]
    block = min(rows, 256)
    count = len(gates)
    return pl.pallas_call(
        hidden_units,
        grid=(rows // block,),
        in_specs=[pl.BlockSpec((block, model // 2), lambda i: (i, 0))] * 2
        + [whole_block(w) for w in gates + ups],
        out_specs=pl.BlockSpec((block, count * width), lambda i: (i, 0)),
        out_shape=jax.ShapeDtypeStruct((rows, count * width), jnp.bfloat16),
        compiler_params=pltpu.CompilerParams(vmem_limit_bytes=40 * 1024 * 1024),
        cost_estimate=pl.CostEstimate(
            flops=4 * rows * model * width * count,
            bytes_accessed=2 * (2 * count * model * width + rows * model),
            transcendentals=0,
        ),
        name="expert_units",
    )(left, right, *gates, *ups)


def weighted_rows(experts, place_ref, share_ref, *refs):
    out_ref = refs[-1]
    acts = jnp.concatenate([ref[...] for ref in refs[:2]], axis=1)
    downs = refs[2:-1]
    width = downs[0].shape[0]
    result = dot(acts[:, :width], downs[0][...])
    for group in range(1, len(downs)):
        result = result + dot(acts[:, group * width : (group + 1) * width], downs[group][...])
    lane = lax.broadcasted_iota(jnp.int32, share_ref.shape, 1)
    chosen = (lane == place_ref[0]) | (lane == place_ref[0] + experts)
    share = jnp.sum(
        jnp.where(chosen, share_ref[...].astype(jnp.float32), 0.0), axis=1, keepdims=True
    )
    out_ref[...] = (result * share).astype(jnp.bfloat16)


def expert_rows(place, gathered, model, experts, acts, downs):
    rows, columns = gathered.shape[0], downs[0].shape[1]
    spare = gathered.shape[1] - model
    block = min(rows, 256)
    return pl.pallas_call(
        functools.partial(weighted_rows, experts),
        grid=(rows // block,),
        in_specs=[
            pl.BlockSpec(memory_space=pltpu.SMEM),
            pl.BlockSpec((block, spare), lambda i: (i, model // spare)),
        ]
        + [pl.BlockSpec((block, act.shape[1]), lambda i: (i, 0)) for act in acts]
        + [whole_block(w) for w in downs],
        out_specs=pl.BlockSpec((block, columns), lambda i: (i, 0)),
        out_shape=jax.ShapeDtypeStruct((rows, columns), jnp.bfloat16),
        compiler_params=pltpu.CompilerParams(vmem_limit_bytes=40 * 1024 * 1024),
        cost_estimate=pl.CostEstimate(
            flops=2 * rows * columns * (acts[0].shape[1] + acts[1].shape[1]),
            bytes_accessed=8_000_000,
            transcendentals=0,
        ),
        name="expert_rows",
    )(place, gathered, *acts, *downs)


def local(
    mix_in, forget_shift, mix_gain, w_query, w_forget, w_value, forget_room, head_gain, w_out,
    moe_in, moe_gain, expert_choice, route_logit, w_exp_gate, w_exp_up, w_exp_down,
    w_sh_gate, w_sh_up, w_sh_down,
):
    tp_count = lax.axis_size("tp")
    rank = lax.axis_index("tp")
    place = lax.axis_index("ep")
    experts = lax.axis_size("ep") * w_exp_gate.shape[0]
    quarter = moe_in.shape[0] // tp_count
    model = moe_in.shape[1]

    half = model // 2
    flat = lambda w: w.reshape(w.shape[1:])
    gates, far_gates = gather_groups(flat(w_exp_gate))
    ups, far_ups = gather_groups(flat(w_exp_up))
    cut = model // 8 * 5
    left_downs = sum(gather_groups(flat(w_exp_down)[:, :cut]), [])
    right_downs = sum(gather_groups(flat(w_exp_down)[:, cut:]), [])

    hidden = norm_rows(moe_in, moe_gain)
    chance = jax.nn.sigmoid(route_logit)
    weights = chance / jnp.sum(chance, axis=-1, keepdims=True) * route_scale
    own_choice = lax.dynamic_slice_in_dim(expert_choice, rank * quarter, quarter, 0)
    table = jnp.sum(
        jnp.where(
            own_choice[..., None] == jnp.arange(experts, dtype=jnp.int32),
            weights[..., None],
            0.0,
        ),
        axis=1,
    )
    high, low = two_part(table)
    spare = -(2 * experts) % 128
    own_rows = lax.dynamic_slice_in_dim(hidden, rank * quarter, quarter, 0)
    sent = jnp.concatenate(
        [own_rows[:, half:], high, low, jnp.zeros((quarter, spare), jnp.bfloat16)], axis=1
    )
    ep_bits = axis_bits("ep")
    turned = ep_bits[1:] + ep_bits[:1]
    far_first = ep_bits[:0:-1]
    left_rows = gather_rows(own_rows[:, :half], "ep", ep_bits[:1] + far_first)
    right_rows = gather_rows(sent, "ep", far_first + ep_bits[:1])

    mixed, query, carry = mixer_scan(
        mix_in, forget_shift, mix_gain, w_query, w_forget, w_value, forget_room
    )
    mixer_part = mixer_finish(mixed, query, carried_blocks(carry), head_gain, w_out)
    shared_gate = jnp.dot(hidden, w_sh_gate, preferred_element_type=jnp.float32)
    shared_up = jnp.dot(hidden, w_sh_up, preferred_element_type=jnp.float32)
    shared_act = (jax.nn.silu(shared_gate) * shared_up).astype(jnp.bfloat16)
    shared_part = jnp.dot(shared_act, w_sh_down, preferred_element_type=jnp.float32)
    tp_bits = axis_bits("tp")
    mixer_held, mixer_bits = halve(split_bits(mixer_part, "tp"), "tp", tp_bits[0])
    shared_held, shared_bits = halve(split_bits(shared_part, "tp"), "tp", tp_bits[0])
    mixer_held, shared_held = mixer_held.astype(jnp.bfloat16), shared_held.astype(jnp.bfloat16)

    left_rows, right_rows, mixer_held, shared_held = lax.optimization_barrier(
        (left_rows, right_rows, mixer_held, shared_held)
    )
    home_act = expert_units(left_rows, right_rows, gates, ups)
    away_act = expert_units(left_rows, right_rows, far_gates, far_ups)
    acts = [home_act, away_act]
    spot = place[None].astype(jnp.int32)
    left = expert_rows(spot, right_rows, half, experts, acts, left_downs)
    right = expert_rows(spot, right_rows, half, experts, acts, right_downs)

    right, mixer_held, shared_held = lax.optimization_barrier((right, mixer_held, shared_held))
    left = scatter_rows(left, "ep", ep_bits)
    right = scatter_rows(right, "ep", turned)
    mixer_sum = halve_all((mixer_held, mixer_bits), "tp", tp_bits[1:])
    shared_sum = halve_all((shared_held, shared_bits), "tp", tp_bits[1:])
    routed = jnp.concatenate([left, right], axis=1)
    return (mixer_sum.astype(jnp.bfloat16), (routed + shared_sum).astype(jnp.bfloat16))


def solution(mesh):
    return jax.shard_map(
        local,
        mesh=mesh,
        in_specs=(
            P("ep", None),
            P("ep"),
            P(),
            P(None, "tp"),
            P(None, "tp"),
            P(None, "tp"),
            P("tp"),
            P("tp"),
            P("tp", None),
            P("ep", None),
            P(),
            P("ep", None),
            P(("ep", "tp"), None),
            P("ep", None, "tp"),
            P("ep", None, "tp"),
            P("ep", "tp", None),
            P(None, "tp"),
            P(None, "tp"),
            P("tp", None),
        ),
        out_specs=(P(("ep", "tp"), None), P(("ep", "tp"), None)),
        check_vma=False,
    )
```
